32 devices in a mesh: tp: 8 (over z, x), dp: 4 (over y, core).
Axes of the slice: x: 2, y: 2, z: 4, core: 2. Of those that a mesh axis runs over, the one named last changes fastest.
Arguments:
- tokens: bfloat16 [128, 4096], P('tp', 'dp'), may hold values from -6 to 6
- query_weight: bfloat16 [2, 4096, 2048], P(None, 'dp', 'tp'), may hold values from -0.09375 to 0.09375
- key_weight: bfloat16 [2, 4096, 2048], P(None, 'dp', 'tp'), may hold values from -0.09375 to 0.09375
- value_weight: bfloat16 [2, 4096, 2048], P(None, 'dp', 'tp'), may hold values from -0.09375 to 0.09375
- outgate_weight: bfloat16 [2, 4096, 2048], P(None, 'dp', 'tp'), may hold values from -0.09375 to 0.09375
- igate_weight: bfloat16 [2, 4096, 16], replicated, may hold values from -0.09375 to 0.09375
- fgate_weight: bfloat16 [2, 4096, 16], replicated, may hold values from -0.09375 to 0.09375
- norm_gain: float32 [2, 4096], P(None, 'dp'), may hold values from 0.1 to 1.9
- head_gain: float32 [2, 2048], P(None, 'tp'), may hold values from 0.1 to 1.9
- proj_weight: bfloat16 [2, 2048, 4096], P(None, 'tp', 'dp'), may hold values from -0.125 to 0.125
- cell_state: float32 [2, 128, 16, 128, 128], P(None, 'dp', 'tp'), may hold values from -1.8 to 1.8
- normer_state: float32 [2, 128, 16, 128], P(None, 'dp', 'tp'), may hold values from -1.8 to 1.8
- stab_state: float32 [2, 128, 16], P(None, 'dp', 'tp'), may hold values from -4 to 4
Outputs:
- final_rows: bfloat16 [128, 4096], P('tp', 'dp')
- cell_out: float32 [2, 128, 16, 128, 128], P(None, 'dp', 'tp')
- normer_out: float32 [2, 128, 16, 128], P(None, 'dp', 'tp')
- stab_out: float32 [2, 128, 16], P(None, 'dp', 'tp')
The draws below stay inside these ranges and needn't reach their ends.
All inputs are finite; a program needn't handle non-finite values.
Results may differ from the reference program's by a relative error of at most 0.012.
The reference program's roundings to bfloat16 on the way count: a program that leaves them out, or rounds other values in their place, can miss the bound.
Values may be sent and summed in bfloat16 or wider, within the bound.
No kernel may reach another device: no remote copies, remote signals or barrier semaphores. Data moves between devices by JAX's collectives and lax.ppermute only.
A program may use at most 64 MiB of HBM per device.

```python
import jax
import jax.numpy as jnp
from jax import lax

D = 4096
HEADS = 16
DH = 128
BLOCKS = 2
INNER = 2048
BATCH = 128


def block_levels(own_key, dims, shards, least, top_value):
    def one(axis_at, shards_of):
        draws = jax.random.uniform(jax.random.fold_in(jax.random.fold_in(own_key, 6), axis_at), (shards_of,), jnp.float32, least / len(shards), top_value / len(shards))
        return jnp.repeat(jnp.exp(draws), dims[axis_at] // shards_of).reshape((-1,) + (1,) * (len(dims) - axis_at - 1))

    gain = one(*shards[0])
    for cut in shards[1:]:
        gain = gain * one(*cut)
    return gain


def centred(key, extent, deviation, bound, split=(), held_as=jnp.bfloat16):
    entries = deviation * jax.random.normal(key, extent, jnp.float32)
    if split:
        entries = entries * block_levels(key, extent, split, -0.22, 0.18)
    return jnp.clip(entries, -bound, bound).astype(held_as)


def setup_inputs(seed: int = 0) -> dict:
    key_of = jax.random.split(jax.random.key(seed), 14)
    return {
        "tokens": centred(key_of[0], (BATCH, D), 1.0, 6.0, ((0, 8), (1, 4))),
        "query_weight": centred(key_of[1], (BLOCKS, D, INNER), D ** -0.5, 0.09375, ((1, 4), (2, 8))),
        "key_weight": centred(key_of[2], (BLOCKS, D, INNER), D ** -0.5, 0.09375, ((1, 4), (2, 8))),
        "value_weight": centred(key_of[3], (BLOCKS, D, INNER), D ** -0.5, 0.09375, ((1, 4), (2, 8))),
        "outgate_weight": centred(key_of[4], (BLOCKS, D, INNER), D ** -0.5, 0.09375, ((1, 4), (2, 8))),
        "igate_weight": centred(key_of[5], (BLOCKS, D, HEADS), D ** -0.5, 0.09375),
        "fgate_weight": centred(key_of[6], (BLOCKS, D, HEADS), D ** -0.5, 0.09375),
        "norm_gain": jnp.clip(1.0 + 0.18 * jax.random.normal(key_of[7], (BLOCKS, D), jnp.float32), 0.1, 1.9),
        "head_gain": jnp.clip(1.0 + 0.18 * jax.random.normal(key_of[8], (BLOCKS, INNER), jnp.float32), 0.1, 1.9),
        "proj_weight": centred(key_of[9], (BLOCKS, INNER, D), INNER ** -0.5, 0.125, ((1, 8), (2, 4))),
        "cell_state": centred(key_of[10], (BLOCKS, BATCH, HEADS, DH, DH), 0.3, 1.8, ((1, 4), (2, 8)), jnp.float32),
        "normer_state": centred(key_of[11], (BLOCKS, BATCH, HEADS, DH), 0.3, 1.8, ((1, 4), (2, 8)), jnp.float32),
        "stab_state": centred(key_of[12], (BLOCKS, BATCH, HEADS), 1.0, 4.0, ((1, 4), (2, 8)), jnp.float32),
    }


EPSILON = 1e-06

def reference(tokens, query_weight, key_weight, value_weight, outgate_weight, igate_weight, fgate_weight, norm_gain, head_gain, proj_weight, cell_state, normer_state, stab_state):
    current = tokens
    batch_rows = tokens.shape[0]
    cell_list = []
    normer_list = []
    stab_list = []
    for layer_num in range(BLOCKS):
        as_float = current.astype(jnp.float32)
        inv_rms = lax.rsqrt(lax.optimization_barrier(jnp.mean(as_float * as_float, axis=1, keepdims=True)) + EPSILON)
        scaled = (as_float * norm_gain[layer_num].astype(jnp.float32)).astype(jnp.bfloat16)

        def product(weight):
            return jnp.dot(scaled, weight, preferred_element_type=jnp.float32) * inv_rms
        query_rows = product(query_weight[layer_num]).reshape(batch_rows, HEADS, DH)
        key_rows = (product(key_weight[layer_num]) * DH ** (-0.5)).reshape(batch_rows, HEADS, DH)
        value_rows = product(value_weight[layer_num]).reshape(batch_rows, HEADS, DH)
        outgate = product(outgate_weight[layer_num])
        igate = product(igate_weight[layer_num])
        forget = jax.nn.log_sigmoid(product(fgate_weight[layer_num]))
        prev_stab = stab_state[layer_num]
        new_stab = jnp.maximum(forget + prev_stab, igate)
        keep_rate = jnp.exp(forget + prev_stab - new_stab)
        write_rate = jnp.exp(igate - new_stab)
        new_cell = keep_rate[..., None, None] * cell_state[layer_num] + write_rate[..., None, None] * value_rows[..., :, None] * key_rows[..., None, :]
        new_normer = keep_rate[..., None] * normer_state[layer_num] + write_rate[..., None] * key_rows
        numerator = jnp.einsum('bhvd,bhd->bhv', new_cell, query_rows, precision=lax.Precision.HIGHEST)
        denominator = jnp.maximum(jnp.abs(lax.optimization_barrier(jnp.sum(new_normer * query_rows, axis=-1))), 1.0)
        readout = numerator / denominator[..., None]
        normed = readout * lax.rsqrt(lax.optimization_barrier(jnp.mean(readout * readout, axis=-1, keepdims=True)) + EPSILON)
        normed = normed * head_gain[layer_num].reshape(HEADS, DH)
        gated_out = (jax.nn.sigmoid(outgate) * normed.reshape(batch_rows, HEADS * DH)).astype(jnp.bfloat16)
        current = jnp.dot(gated_out, proj_weight[layer_num], preferred_element_type=jnp.float32).astype(jnp.bfloat16)
        cell_list.append(new_cell)
        normer_list.append(new_normer)
        stab_list.append(new_stab)
    return (current, jnp.stack(cell_list), jnp.stack(normer_list), jnp.stack(stab_list))
```

```python
import functools

import jax
import jax.numpy as jnp
from jax import lax
from jax.experimental import pallas as pl
from jax.experimental.pallas import tpu as pltpu
from jax.sharding import PartitionSpec as P

EPSILON = 1e-06
LANES = 128
F32 = jnp.float32
BF16 = jnp.bfloat16


def inner_size(size):
    inner = 1
    while (inner * 2) ** 2 <= size:
        inner *= 2
    return inner


class Ring:
    def __init__(self, axis, size, stride, count):
        self.axis = axis
        self.size = size
        self.stride = stride
        self.count = count
        self.rank = (lax.axis_index(axis) // stride) % count

    def send(self, value, step):
        pairs = []
        for src in range(self.size):
            digit = (src // self.stride) % self.count
            pairs.append((src, src + ((digit ^ step) - digit) * self.stride))
        return lax.ppermute(value, self.axis, pairs)

    def gather(self, value):
        buf = jnp.zeros((self.count,) + value.shape, value.dtype)
        buf = lax.dynamic_update_index_in_dim(buf, value, self.rank, 0)
        got = [self.send(value, step) for step in range(1, self.count)]
        for step in range(1, self.count):
            buf = lax.dynamic_update_index_in_dim(buf, got[step - 1], self.rank ^ step, 0)
        return buf

    def scatter(self, chunks):
        return self.exchange([lax.dynamic_index_in_dim(chunks, self.rank ^ step, 0, False) for step in range(self.count)])

    def exchange(self, parts):
        return [parts[0]] + [self.send(parts[step], step) for step in range(1, self.count)]


def split(value):
    high = value.astype(BF16).astype(F32)
    return high, value - high


def project_kernel(layer, rank_ref, g_ref, gain_ref, wq_ref, wk_ref, wv_ref, wo_ref, wg_ref, *refs):
    out_refs, all_ref = refs[:-1], refs[-1]
    chunks, rows, _ = all_ref.shape
    width = wq_ref.shape[2]
    cols = wg_ref.shape[2]
    as_float = g_ref[...].astype(F32)
    squares = jnp.sum(as_float * as_float, axis=1, keepdims=True)
    scaled = (as_float * gain_ref[layer : layer + 1, :]).astype(BF16)

    def put(at, part):
        all_ref[:, :, at : at + part.shape[1]] = part.astype(BF16).reshape(chunks, rows, part.shape[1])

    for num, w_ref in enumerate((wq_ref, wk_ref, wv_ref, wo_ref)):
        part = jnp.dot(scaled, w_ref[0], preferred_element_type=F32)
        put(num * width, part)
        put(4 * width + cols + num * width, split(part)[1])
    extra = jnp.dot(scaled, wg_ref[0], preferred_element_type=F32)
    lane = lax.broadcasted_iota(jnp.int32, extra.shape, 1)
    extra = jnp.where(lane == cols // 2 - 1, squares, extra)
    high, low = split(extra)
    put(4 * width, jnp.where(lane < cols // 2, high, pltpu.roll(low, cols // 2, 1)))
    for step, out_ref in enumerate(out_refs):
        out_ref[...] = all_ref[rank_ref[0] ^ step]


def project(layer, chunks, rank, gathered, norm_gain, weights, gate_weight):
    batch, row_width = gathered.shape
    width = weights[0].shape[2]
    cols = gate_weight.shape[2]
    total = 8 * width + cols
    rows = batch // chunks
    weight_spec = pl.BlockSpec((1, row_width, width), lambda i, r: (layer, 0, 0))
    return pl.pallas_call(
        functools.partial(project_kernel, layer),
        grid_spec=pltpu.PrefetchScalarGridSpec(
            num_scalar_prefetch=1,
            grid=(1,),
            in_specs=[
                pl.BlockSpec((batch, row_width), lambda i, r: (0, 0)),
                pl.BlockSpec(norm_gain.shape, lambda i, r: (0, 0)),
                weight_spec,
                weight_spec,
                weight_spec,
                weight_spec,
                pl.BlockSpec((1, row_width, cols), lambda i, r: (layer, 0, 0)),
            ],
            out_specs=[pl.BlockSpec((rows, total), lambda i, r: (0, 0))] * chunks,
            scratch_shapes=[pltpu.VMEM((chunks, rows, total), BF16)],
        ),
        out_shape=[jax.ShapeDtypeStruct((rows, total), BF16)] * chunks,
        cost_estimate=pl.CostEstimate(
            flops=2 * batch * row_width * total, bytes_accessed=2 * row_width * total, transcendentals=0
        ),
        name="project",
    )(rank.reshape((1,)).astype(jnp.int32), gathered, norm_gain, *weights, gate_weight)


def state_kernel(layer, model_width, num_parts, step_rows, *refs):
    parts = refs[:num_parts]
    gain_ref, cell_ref, normer_ref, stab_ref = refs[num_parts : num_parts + 4]
    gated_ref, cell_out, normer_out, stab_out, sum_ref, gate_ref = refs[-6:]
    step = pl.program_id(0)
    heads, head_dim = normer_ref.shape[2], normer_ref.shape[3]
    width = heads * head_dim
    cols = sum_ref.shape[1] - 4 * width
    total_width = sum_ref.shape[1]

    @pl.when(step == 0)
    def _():
        total = parts[0][...].astype(F32)
        for part in parts[1:]:
            total = total + part[...].astype(F32)
        sum_ref[:, : 4 * width] = total[:, : 4 * width] + total[:, total_width:]
        sum_ref[:, 4 * width :] = total[:, 4 * width : total_width]

    here = pl.ds(pl.multiple_of(step * step_rows, step_rows), step_rows)
    extra = sum_ref[here, 4 * width : 4 * width + cols]
    extra = extra + pltpu.roll(extra, cols // 2, 1)
    square = extra[:, cols // 2 - 1 : cols // 2]
    inv_rms = lax.rsqrt(square / model_width + EPSILON)
    igate = extra[:, :heads] * inv_rms
    forget = extra[:, heads : 2 * heads] * inv_rms
    forget = jnp.minimum(forget, 0.0) - jnp.log1p(jnp.exp(-jnp.abs(forget)))
    carried = forget + stab_ref[0]
    new_stab = jnp.maximum(carried, igate)
    keep_rate = jnp.exp(carried - new_stab)
    write_rate = jnp.exp(igate - new_stab)
    stab_out[0] = new_stab
    lane = lax.broadcasted_iota(jnp.int32, (head_dim, 2 * step_rows), 1) % step_rows
    spread = (step_rows, step_rows * head_dim)
    diagonal = lax.broadcasted_iota(jnp.int32, spread, 0) == lax.broadcasted_iota(jnp.int32, spread, 1) // head_dim
    for head in range(heads):
        def rows(num):
            start = num * width + head * head_dim
            return sum_ref[here, start : start + head_dim] * inv_rms

        query, key, value, outgate = rows(0), rows(1) * head_dim ** (-0.5), rows(2), rows(3)
        keep = keep_rate[:, head : head + 1]
        write = write_rate[:, head : head + 1]
        new_normer = keep * normer_ref[0, :, head, :] + write * key
        normer_out[0, :, head, :] = new_normer
        value_high, value_low = split(write * value)
        tiled = jnp.where(diagonal, jnp.concatenate([key] * step_rows, axis=1), 0.0)
        key_high, key_low = split(tiled)
        outer = jnp.dot(
            jnp.concatenate([value_high, value_low, value_high], axis=0).T.astype(BF16),
            jnp.concatenate([key_high, key_high, key_low], axis=0).astype(BF16),
            preferred_element_type=F32,
        )
        columns = jnp.concatenate(split(query), axis=0).T.astype(BF16)
        columns = jnp.concatenate([columns, columns], axis=0)
        numerator = jnp.zeros((head_dim, 2 * step_rows), F32)
        for seq in range(step_rows):
            new_cell = (
                keep[seq : seq + 1] * cell_ref[0, seq, head] + outer[:, seq * head_dim : (seq + 1) * head_dim]
            )
            cell_out[0, seq, head] = new_cell
            high = new_cell.astype(BF16)
            low = (new_cell - high.astype(F32)).astype(BF16)
            product = jnp.dot(jnp.concatenate([high, low], axis=1), columns, preferred_element_type=F32)
            numerator = jnp.where(lane == seq, product, numerator)
        numerator = numerator.T
        numerator = numerator[:step_rows] + numerator[step_rows:]
        denominator = jnp.maximum(
            jnp.abs(jnp.sum(new_normer * query, axis=1, keepdims=True)), 1.0
        )
        readout = numerator / denominator
        normed = readout * lax.rsqrt(jnp.mean(readout * readout, axis=1, keepdims=True) + EPSILON)
        normed = normed * gain_ref[layer : layer + 1, head * head_dim : (head + 1) * head_dim]
        gate_ref[here, head * head_dim : (head + 1) * head_dim] = jax.nn.sigmoid(outgate) * normed

    @pl.when(step == pl.num_programs(0) - 1)
    def _():
        gated_ref[...] = gate_ref[...].astype(BF16)


def update_state(layer, model_width, parts, head_gain, cell, normer, stab, earlier):
    seqs, heads, head_dim = normer.shape[1:]
    step_rows = min(8, seqs)
    cell_spec = pl.BlockSpec((1, step_rows, heads, head_dim, head_dim), lambda i: (layer, i, 0, 0, 0))
    normer_spec = pl.BlockSpec((1, step_rows, heads, head_dim), lambda i: (layer, i, 0, 0))
    stab_spec = pl.BlockSpec((1, step_rows, heads), lambda i: (layer, i, 0))
    whole = lambda shape: pl.BlockSpec(shape, lambda i: (0,) * len(shape))
    num = len(parts)
    return pl.pallas_call(
        functools.partial(state_kernel, layer, model_width, num, step_rows),
        grid=(seqs // step_rows,),
        in_specs=[whole(part.shape) for part in parts]
        + [whole(head_gain.shape), cell_spec, normer_spec, stab_spec]
        + [pl.BlockSpec(memory_space=pl.ANY)] * len(earlier),
        out_specs=[whole((seqs, heads * head_dim)), cell_spec, normer_spec, stab_spec],
        out_shape=[
            jax.ShapeDtypeStruct((seqs, heads * head_dim), BF16),
            jax.ShapeDtypeStruct(cell.shape, F32),
            jax.ShapeDtypeStruct(normer.shape, F32),
            jax.ShapeDtypeStruct(stab.shape, F32),
        ],
        scratch_shapes=[
            pltpu.VMEM((seqs, parts[0].shape[1] - 4 * heads * head_dim), F32),
            pltpu.VMEM((seqs, heads * head_dim), F32),
        ],
        input_output_aliases={num + 4 + at: 1 + at for at in range(len(earlier))},
        cost_estimate=pl.CostEstimate(
            flops=8 * seqs * heads * head_dim * head_dim,
            bytes_accessed=8 * seqs * heads * head_dim * head_dim,
            transcendentals=0,
        ),
        compiler_params=pltpu.CompilerParams(dimension_semantics=("arbitrary",)),
        name="state",
    )(*parts, head_gain, cell, normer, stab, *earlier)


def add(parts, held_as):
    total = parts[0].astype(F32)
    for part in parts[1:]:
        total = total + part.astype(F32)
    return total.astype(held_as)


def per_device(
    tp_size,
    dp_size,
    tokens,
    query_weight,
    key_weight,
    value_weight,
    outgate_weight,
    igate_weight,
    fgate_weight,
    norm_gain,
    head_gain,
    proj_weight,
    cell_state,
    normer_state,
    stab_state,
):
    dp_rank = lax.axis_index("dp")
    tp_rank = lax.axis_index("tp")
    num_blocks, seqs, heads = stab_state.shape
    row_width = query_weight.shape[1]
    inner = inner_size(tp_size)
    near = Ring("tp", tp_size, 1, inner)
    far = Ring("tp", tp_size, inner, tp_size // inner)
    across = Ring("dp", dp_size, 1, dp_size)
    own_rows = tokens.shape[0]

    start = (0, dp_rank * row_width, tp_rank * heads)
    extent = (num_blocks, row_width, heads)
    gate_weight = jnp.concatenate(
        [lax.dynamic_slice(igate_weight, start, extent), lax.dynamic_slice(fgate_weight, start, extent)], axis=2
    )
    gate_weight = jnp.pad(gate_weight, ((0, 0), (0, 0), (0, LANES - 2 * heads)))
    weights = (query_weight, key_weight, value_weight, outgate_weight)

    def rows_of(stacked):
        return stacked.reshape((-1, stacked.shape[-1]))

    gathered = rows_of(far.gather(rows_of(near.gather(tokens))))
    earlier = ()
    for layer in range(num_blocks):
        parts = across.exchange(project(layer, dp_size, dp_rank, gathered, norm_gain, weights, gate_weight))
        gated, *earlier = update_state(
            layer, row_width * dp_size, parts, head_gain, cell_state, normer_state, stab_state, earlier
        )
        all_gated = rows_of(across.gather(gated))
        last = layer + 1 == num_blocks
        sent_as = BF16 if last else F32
        out_part = jnp.dot(all_gated, proj_weight[layer], preferred_element_type=F32).astype(sent_as)
        out_part = out_part.reshape(tp_size // inner, inner * own_rows, -1)
        summed = add(far.scatter(out_part), sent_as)
        if last:
            final_rows = add(near.scatter(summed.reshape(inner, own_rows, -1)), BF16)
        else:
            summed = add([summed] + [near.send(summed, step) for step in range(1, inner)], BF16)
            gathered = rows_of(far.gather(summed))
    return (final_rows, *earlier)


def solution(mesh):
    return jax.shard_map(
        functools.partial(per_device, mesh.shape["tp"], mesh.shape["dp"]),
        mesh=mesh,
        in_specs=(
            P("tp", "dp"),
            P(None, "dp", "tp"),
            P(None, "dp", "tp"),
            P(None, "dp", "tp"),
            P(None, "dp", "tp"),
            P(),
            P(),
            P(None, "dp"),
            P(None, "tp"),
            P(None, "tp", "dp"),
            P(None, "dp", "tp", None, None),
            P(None, "dp", "tp", None),
            P(None, "dp", "tp"),
        ),
        out_specs=(
            P("tp", "dp"),
            P(None, "dp", "tp", None, None),
            P(None, "dp", "tp", None),
            P(None, "dp", "tp"),
        ),
        check_vma=False,
    )
```
